32 devices in a mesh: sp: 8 (over z, x), tp: 4 (over y, core).
Axes of the slice: x: 2, y: 2, z: 4, core: 2. Of those that a mesh axis runs over, the one named last changes fastest.
Arguments:
- residual_in: bfloat16 [4096, 2048], P('sp'), may hold values from -6 to 6
- gate_in: bfloat16 [4096, 2048], P('sp', 'tp'), may hold values from -6 to 6
- value_in: bfloat16 [4096, 2048], P('sp', 'tp'), may hold values from -6 to 6
- conv_weight: float32 [4, 2048], P(None, 'tp'), may hold values from -3 to 3
- rate_weight: bfloat16 [32, 64, 64], P('tp'), may hold values from -0.75 to 0.75
- input_weight: bfloat16 [32, 64, 64], P('tp'), may hold values from -0.75 to 0.75
- decay_base: float32 [2048], P('tp'), may hold values from 3.0517578e-06 to 0.015, as said below
- step_scale: float32 [4096, 2048], P('sp', 'tp'), may hold values from 0.25 to 57344, as said below
- out_weight: bfloat16 [2048, 2048], P('tp'), may hold values from -0.375 to 0.375
- norm_gain: float32 [2048], replicated, may hold values from 0.1 to 1.9
- up_weight: bfloat16 [2048, 8192], P('sp', 'tp'), may hold values from -0.125 to 0.125
- down_weight: bfloat16 [2048, 8192], P('sp', 'tp'), may hold values from -0.0625 to 0.0625
Outputs:
- block_out: bfloat16 [4096, 2048], P(('sp', 'tp'))
The draws below stay inside these ranges and needn't reach their ends.
Inputs may be any that keep to these rules, and one draw needn't show every extreme that they name: `decay_base`: positive. `step_scale`: positive.
All inputs are finite; a program needn't handle non-finite values.
Results may differ from the reference program's by a relative error of at most 0.018.
Values may be sent and summed in bfloat16 or wider, within the bound.
A program may use at most 128 MiB of HBM per device.

```python
import jax
import jax.numpy as jnp
from jax import lax

D = 2048
BW = 64
FF = 8192
CONV = 4
TOK_DEV = 512
R = 2048
BLOCKS = 32
RCH = 512
FCH = 2048
TOKENS = 4096
N_TP = 4


def channel_law(key):
    base_key = jax.random.fold_in(key, 11)
    pick_key, slow_key, fast_key = jax.random.split(base_key, 3)
    slow_mask = jax.random.bernoulli(pick_key, 0.5, (R,))
    slow_rate = jax.random.uniform(slow_key, (R,), jnp.float32, 0.05, 0.5) / (4.0 * TOKENS)
    fast_rate = jax.random.uniform(fast_key, (R,), jnp.float32, 0.005, 0.015)
    return jnp.where(slow_mask, slow_rate, fast_rate)


def draw_decay_base(key, part):
    return channel_law(key)


def draw_step_scale(key, part):
    per_channel_rate = channel_law(key)
    scale_key = jax.random.fold_in(key, 23)
    level_key, rough_key, spot_key, loss_key = jax.random.split(scale_key, 4)
    block_total = TOKENS // TOK_DEV
    noise_level = jnp.exp(jax.random.uniform(level_key, (block_total, 1), jnp.float32, -0.6931, 0.6931))
    noise_level = jnp.repeat(noise_level, TOK_DEV, axis=0)
    noisy_input = jax.random.uniform(rough_key, (TOKENS, R), jnp.float32, 0.5, 1.5)
    spots = jax.random.randint(spot_key, (8,), 0, TOKENS)
    flagged_rows = jnp.zeros((TOKENS,), jnp.float32).at[spots].set(1.0)
    training_loss = jax.random.uniform(loss_key, (TOKENS, R), jnp.float32, 0.25, 0.7)
    spike_draw = training_loss / (4.0 * per_channel_rate[None, :])
    return jnp.where(flagged_rows[:, None] > 0.5, spike_draw, noise_level * noisy_input)


def block_levels(key, shape, pieces, smallest, top_value):
    def one(dim, parts):
        steps = jax.random.uniform(jax.random.fold_in(jax.random.fold_in(key, 6), dim), (parts,), jnp.float32, smallest / len(pieces), top_value / len(pieces))
        return jnp.repeat(jnp.exp(steps), shape[dim] // parts).reshape((-1,) + (1,) * (len(shape) - dim - 1))

    gain = one(*pieces[0])
    for cut in pieces[1:]:
        gain = gain * one(*cut)
    return gain


def bell_draw(stream_key, dims, deviation, reach, cuts=(), kind=jnp.bfloat16):
    result = jax.random.normal(stream_key, dims, jnp.float32) * deviation
    if len(cuts) > 0:
        result = block_levels(stream_key, dims, cuts, -0.22, 0.18) * result
    return jnp.clip(result, min=-reach, max=reach).astype(kind)


def setup_inputs(seed: int = 0) -> dict:
    key_list = jax.random.split(jax.random.key(seed), 13)
    return {
        "residual_in": bell_draw(key_list[0], (TOKENS, D), 1.0, 6.0, ((0, 8),)),
        "gate_in": bell_draw(key_list[1], (TOKENS, R), 1.0, 6.0, ((0, 8), (1, 4))),
        "value_in": bell_draw(key_list[2], (TOKENS, R), 1.0, 6.0, ((0, 8), (1, 4))),
        "conv_weight": bell_draw(key_list[3], (CONV, R), CONV ** -0.5, 3.0, ((1, 4),), jnp.float32),
        "rate_weight": bell_draw(key_list[4], (BLOCKS, BW, BW), BW ** -0.5, 0.75, ((0, 4),)),
        "input_weight": bell_draw(key_list[5], (BLOCKS, BW, BW), BW ** -0.5, 0.75, ((0, 4),)),
        "decay_base": draw_decay_base(jax.random.fold_in(key_list[12], 71), 0),
        "step_scale": draw_step_scale(jax.random.fold_in(key_list[12], 71), 0),
        "out_weight": bell_draw(key_list[8], (R, D), (R // 8) ** -0.5, 0.375, ((0, 4),)),
        "norm_gain": jnp.clip(1.0 + 0.18 * jax.random.normal(key_list[9], (D,), jnp.float32), 0.1, 1.9),
        "up_weight": bell_draw(key_list[10], (D, FF), D ** -0.5, 0.125, ((0, 8), (1, 4))),
        "down_weight": bell_draw(key_list[11], (D, FF), FF ** -0.5, 0.0625, ((0, 8), (1, 4))),
    }


def chain_join(earlier, later):
    return (earlier[0] * later[0], later[0] * earlier[1] + later[1])

def rounded(term):
    return lax.optimization_barrier(term.astype(jnp.bfloat16)).astype(jnp.float32)

def reference(residual_in, gate_in, value_in, conv_weight, rate_weight, input_weight, decay_base, step_scale, out_weight, norm_gain, up_weight, down_weight):
    tap_count = conv_weight.shape[0]
    total_rows = value_in.shape[0]
    padded = jnp.pad(value_in.astype(jnp.float32), ((tap_count - 1, 0), (0, 0)))
    filtered_rows = jnp.zeros(value_in.shape, jnp.float32)
    for offset in range(tap_count):
        filtered_rows = filtered_rows + padded[offset:offset + total_rows] * conv_weight[offset]
    smoothed = filtered_rows.astype(jnp.bfloat16)
    grouped = smoothed.astype(jnp.float32).reshape(total_rows, BLOCKS, BW)
    rate_gate = jax.nn.sigmoid(jnp.einsum('tnd,nde->tne', grouped, rate_weight.astype(jnp.float32))).reshape(total_rows, R)
    input_gate = jax.nn.sigmoid(jnp.einsum('tnd,nde->tne', grouped, input_weight.astype(jnp.float32))).reshape(total_rows, R)
    log_keep = -8.0 * step_scale * rate_gate * decay_base[None, :]
    drive = jnp.sqrt(-jnp.expm1(2.0 * log_keep)) * input_gate * smoothed.astype(jnp.float32)
    products, carry_state = lax.associative_scan(chain_join, (jnp.exp(log_keep), drive), axis=0)
    gated = (jax.nn.gelu(gate_in.astype(jnp.float32), approximate=True) * carry_state).astype(jnp.bfloat16)
    mixed = jnp.zeros((total_rows, D), jnp.float32)
    for group in range(N_TP):
        part_sum = jnp.dot(gated[:, group * RCH:(group + 1) * RCH], out_weight[group * RCH:(group + 1) * RCH], preferred_element_type=jnp.float32)
        mixed = mixed + rounded(part_sum)
    updated = (residual_in.astype(jnp.float32) + mixed).astype(jnp.bfloat16)
    widened = updated.astype(jnp.float32)
    factor = lax.rsqrt(lax.optimization_barrier(jnp.mean(widened * widened, axis=-1, keepdims=True)) + 1e-06)
    normed = (widened * factor * norm_gain).astype(jnp.bfloat16)
    down_sum = jnp.zeros((total_rows, D), jnp.float32)
    for group in range(N_TP):
        lifted = jnp.dot(normed, up_weight[:, group * FCH:(group + 1) * FCH], preferred_element_type=jnp.float32)
        activated = jnp.square(jax.nn.relu(lifted)).astype(jnp.bfloat16)
        part_sum = lax.dot_general(activated, down_weight[:, group * FCH:(group + 1) * FCH], (((1,), (1,)), ((), ())), preferred_element_type=jnp.float32)
        down_sum = down_sum + rounded(part_sum)
    return (updated.astype(jnp.float32) + down_sum).astype(jnp.bfloat16)
```

```python
import functools

import jax
import jax.numpy as jnp
from jax import lax
from jax.experimental import pallas as pl
from jax.experimental.pallas import tpu as pltpu
from jax.sharding import PartitionSpec as P

MESH = pl.DeviceIdType.MESH
F32 = jnp.float32
BF16 = jnp.bfloat16
SCAN = 8


def one_minus_exp(y):
    series = 1.0 + y * (1.0 / 7.0)
    for n in (6.0, 5.0, 4.0, 3.0, 2.0):
        series = 1.0 + y * (1.0 / n) * series
    return jnp.where(y > -0.3, -y * series, 1.0 - jnp.exp(y))


def kernel(
    dims,
    res_hbm, gate_hbm, value_hbm, conv_ref, rate_ref, inp_ref, decay_ref, step_hbm,
    outw_hbm, gain_ref, up_hbm, down_hbm,
    out_ref,
    up_all, down_all, acc, act, normed, part, part_in, fin, fin_in,
    keep, drive, pad, gated, gate_v, value_v, step_v, outw_v, res_v, halo, tot, ent,
    upd, wpair, send, recv, tsend, trecv, csend, crecv, local_sem,
):
    n_sp, n_tp, ids = dims
    me, tp = lax.axis_index("sp"), lax.axis_index("tp")
    high = n_sp // 2
    hi, lo = me // 2, lax.rem(me, 2)
    rows, ch = value_v.shape
    width = up_all.shape[0]
    hidden = up_all.shape[1]
    piece = up_hbm.shape[0]
    own = rows // n_tp
    last = high // 2

    def at(step, side):
        low = lo if side == "o" else 1 - lo
        return lax.rem(hi + step + 2 * high, high) * 2 + low

    beside, above, below = at(0, "x"), at(1, "o"), at(-1, "o")

    loads = {}
    for n, (key, src, dst) in enumerate(
        (
            ("value", value_hbm, value_v),
            ("step", step_hbm, step_v),
            ("gate", gate_hbm, gate_v),
            ("outw", outw_hbm, outw_v),
            ("res", res_hbm.at[pl.ds(pl.multiple_of(tp * own, own), own), :], res_v),
            ("up", up_hbm, up_all.at[pl.ds(pl.multiple_of(me * piece, piece), piece), :]),
            ("down", down_hbm, down_all.at[pl.ds(pl.multiple_of(me * piece, piece), piece), :]),
        )
    ):
        loads[key] = pltpu.make_async_copy(src, dst, local_sem.at[n])
        loads[key].start()

    barrier = pltpu.get_barrier_semaphore()
    for d in range(1, n_sp):
        pl.semaphore_signal(
            barrier, inc=1, device_id=(lax.rem(me + d, n_sp), tp), device_id_type=MESH
        )
    for d in range(1, n_tp):
        pl.semaphore_signal(
            barrier, inc=1, device_id=(me, lax.rem(tp + d, n_tp)), device_id_type=MESH
        )
    pl.semaphore_wait(barrier, n_sp + n_tp - 2)

    started = {}

    def launch(key, src, dst, target):
        copy = pltpu.make_async_remote_copy(
            src_ref=src, dst_ref=dst, send_sem=send.at[ids[key]], recv_sem=recv.at[ids[key]],
            device_id=target, device_id_type=MESH,
        )
        copy.start()
        started[key] = copy

    def rows_of(ref, source, half):
        if half is None:
            return ref.at[pl.ds(pl.multiple_of(source * piece, piece), piece), :]
        h = piece // 2
        return ref.at[pl.ds(pl.multiple_of(source * piece + half * h, h), h), :]

    def half_of(k, sign):
        return None if k < last else (0 if sign > 0 else 1)

    def ring(name, hbm, buf, side, k, sign):
        source = at(-sign * (k - 1), side)
        half = half_of(k, sign)
        dst = rows_of(buf, source, half)
        if k == 1 and side == "o":
            h = piece // 2
            src = hbm if half is None else hbm.at[pl.ds(half * h, h), :]
        else:
            src = dst
        launch((name, side, k, sign), src, dst, (above if sign > 0 else below, tp))

    def ring_all(name, hbm, buf, side, k):
        for sign in (1, -1):
            ring(name, hbm, buf, side, k, sign)

    up_x_key, down_x_key = ("ux",), ("dx",)
    halo_copy_key = ("halo",)
    launch(
        halo_copy_key, value_hbm.at[pl.ds(rows - 16, 16), :], halo,
        (lax.rem(me + 1, n_sp), tp),
    )
    ring_all("u", up_hbm, up_all, "o", 1)
    launch(up_x_key, up_hbm, rows_of(up_all, me, None), (beside, tp))
    ring_all("d", down_hbm, down_all, "o", 1)
    launch(down_x_key, down_hbm, rows_of(down_all, me, None), (beside, tp))

    def up_forward(side, k):
        for sign in (1, -1):
            started[("u", side, k, sign)].wait_recv()
            if k < last:
                ring("u", up_hbm, up_all, side, k + 1, sign)

    def down_forward(k):
        for sign in (1, -1):
            started[("d", "o", k, sign)].wait_recv()
            if k < last:
                ring("d", down_hbm, down_all, "o", k + 1, sign)
        for sign in (1, -1):
            view = rows_of(down_all, at(-sign * k, "o"), half_of(k, sign))
            launch(("f", k, sign), view, view, (beside, tp))

    bw = rate_ref.shape[1]
    per = 128 // bw
    groups = ch // 128
    r_i = lax.broadcasted_iota(jnp.int32, (bw, 128), 0)
    c_i = lax.broadcasted_iota(jnp.int32, (bw, 128), 1)
    for g in range(groups):
        for which, ref in ((0, rate_ref), (1, inp_ref)):
            for j in range(per):
                place = jnp.where(c_i == r_i + j * bw, 1.0, 0.0).astype(BF16)
                block = jnp.dot(ref[g * per + j], place, preferred_element_type=F32)
                wpair[which, g, j * bw : (j + 1) * bw, :] = block.astype(BF16)

    loads["value"].wait()
    loads["step"].wait()
    started[halo_copy_key].wait_recv()
    taps = conv_ref.shape[0]
    first = jnp.where(me == 0, 0.0, 1.0).astype(F32)
    pad[0:8, :] = halo[8:16, :].astype(F32) * first

    chunk = 64

    def widen(r, c):
        at_row = pl.multiple_of(r * chunk, chunk)
        pad[pl.ds(pl.multiple_of(at_row + 8, 8), chunk), :] = value_v[
            pl.ds(at_row, chunk), :
        ].astype(F32)
        return c

    lax.fori_loop(0, rows // chunk, widen, 0)

    def gates(r, c):
        at_row = pl.multiple_of(r * chunk, chunk)
        for g in range(groups):
            lanes = slice(g * 128, (g + 1) * 128)
            window = pad[pl.ds(at_row, chunk + 8), lanes]
            total = jnp.zeros((chunk, 128), F32)
            for k in range(taps):
                shift = 8 - taps + 1 + k
                moved = window if shift == 0 else pltpu.roll(window, chunk + 8 - shift, 0)
                total = total + moved[0:chunk, :] * conv_ref[k : k + 1, lanes]
            smooth = total.astype(BF16)
            rate = lax.logistic(jnp.dot(smooth, wpair[0, g], preferred_element_type=F32))
            gate = lax.logistic(jnp.dot(smooth, wpair[1, g], preferred_element_type=F32))
            log_keep = -8.0 * step_v[pl.ds(at_row, chunk), lanes] * rate * decay_ref[0:1, lanes]
            keep[g, pl.ds(at_row, chunk), :] = jnp.exp(log_keep)
            drive[g, pl.ds(at_row, chunk), :] = (
                jnp.sqrt(one_minus_exp(2.0 * log_keep)) * gate * smooth.astype(F32)
            )
        return c

    lax.fori_loop(0, rows // chunk, gates, 0)

    seg = rows // SCAN

    def scan(i, carry):
        p, h = carry
        idx = pl.ds(i, SCAN, stride=seg)
        new_p, new_h = [], []
        for g in range(groups):
            a, d = keep[g, idx, :], drive[g, idx, :]
            hg = a * h[g] + d
            pg = a * p[g]
            keep[g, idx, :] = pg
            drive[g, idx, :] = hg
            new_p.append(pg)
            new_h.append(hg)
        return tuple(new_p), tuple(new_h)

    ones = tuple(jnp.ones((SCAN, 128), F32) for _ in range(groups))
    zeros = tuple(jnp.zeros((SCAN, 128), F32) for _ in range(groups))
    lax.fori_loop(0, seg, scan, (ones, zeros))

    def line(ref, row):
        return jnp.concatenate([ref[g, row : row + 1, :] for g in range(groups)], axis=1)

    ends = [(line(keep, (b + 1) * seg - 1), line(drive, (b + 1) * seg - 1)) for b in range(SCAN)]
    whole_p, whole_h = ends[0]
    for p_b, h_b in ends[1:]:
        whole_p, whole_h = whole_p * p_b, p_b * whole_h + h_b
    row_id = lax.broadcasted_iota(jnp.int32, (8, ch), 0)
    tot[me] = jnp.where(row_id == 0, whole_p, whole_h)
    carries = []
    for d in range(1, n_sp):
        copy = pltpu.make_async_remote_copy(
            src_ref=tot.at[me], dst_ref=tot.at[me], send_sem=csend.at[d], recv_sem=crecv.at[d],
            device_id=(lax.rem(me + d, n_sp), tp), device_id_type=MESH,
        )
        copy.start()
        carries.append(copy)
    loads["gate"].wait()
    loads["outw"].wait()
    for copy in carries:
        copy.wait_recv()

    def fold(d, s):
        joined = tot[d, 0:1, :] * s + tot[d, 1:2, :]
        return jnp.where(d < me, joined, s)

    state = lax.fori_loop(0, n_sp, fold, jnp.zeros((1, ch), F32))
    for b in range(SCAN):
        ent[b, 0:1, :] = state
        state = ends[b][0] * state + ends[b][1]

    def gating(b, c):
        at_row = pl.ds(pl.multiple_of(b * seg, seg), seg)
        for g in range(groups):
            lanes = slice(g * 128, (g + 1) * 128)
            full = drive[g, at_row, :] + keep[g, at_row, :] * ent[b, 0:1, lanes]
            branch = jax.nn.gelu(gate_v[at_row, lanes].astype(F32), approximate=True)
            gated[at_row, lanes] = (branch * full).astype(BF16)
        return c

    lax.fori_loop(0, SCAN, gating, 0)

    sums = []
    for d in list(range(1, n_tp)) + [0]:
        peer = lax.rem(tp + d, n_tp)
        span = pl.ds(pl.multiple_of(peer * own, own), own)
        part[span, :] = jnp.dot(gated[span, :], outw_v[...], preferred_element_type=F32).astype(BF16)
        if d:
            copy = pltpu.make_async_remote_copy(
                src_ref=part.at[span, :], dst_ref=part_in.at[tp],
                send_sem=tsend.at[0, d], recv_sem=trecv.at[0, d],
                device_id=(me, peer), device_id_type=MESH,
            )
            copy.start()
            sums.append(copy)

    started[up_x_key].wait_recv()
    ring_all("u", up_hbm, up_all, "x", 1)
    up_forward("o", 1)

    mine = pl.ds(pl.multiple_of(tp * own, own), own)
    loads["res"].wait()
    for copy in sums:
        copy.wait_recv()
    slab = 32

    def settle(r, c):
        here = pl.ds(pl.multiple_of(r * slab, slab), slab)
        there = pl.ds(pl.multiple_of(tp * own + r * slab, slab), slab)
        mixed = part[there, :].astype(F32)
        for d in range(1, n_tp):
            mixed = mixed + part_in[lax.rem(tp + d, n_tp), here, :].astype(F32)
        new = (res_v[here, :].astype(F32) + mixed).astype(BF16)
        upd[here, :] = new
        wide = new.astype(F32)
        factor = lax.rsqrt(jnp.mean(wide * wide, axis=-1, keepdims=True) + 1e-06)
        normed[there, :] = (wide * factor * gain_ref[0:1, :]).astype(BF16)
        return c

    lax.fori_loop(0, own // slab, settle, 0)
    shares = []
    for d in range(1, n_tp):
        copy = pltpu.make_async_remote_copy(
            src_ref=normed.at[mine, :], dst_ref=normed.at[mine, :],
            send_sem=tsend.at[1, d], recv_sem=trecv.at[1, d],
            device_id=(me, lax.rem(tp + d, n_tp)), device_id_type=MESH,
        )
        copy.start()
        shares.append(copy)

    down_forward(1)
    up_forward("x", 1)
    for k in range(2, last):
        up_forward("o", k)
        down_forward(k)
        up_forward("x", k)
    for copy in shares:
        copy.wait_recv()
    loads["up"].wait()
    loads["down"].wait()

    streaming = piece % 128 == 0
    tile = 512
    tiles = hidden // tile

    def gather_dot(sources, cols):
        total = None
        for s in sources:
            deep = pl.ds(pl.multiple_of(s * piece, piece), piece)
            term = jnp.dot(normed[:, deep], up_all[deep, cols], preferred_element_type=F32)
            total = term if total is None else total + term
        return total

    if streaming:
        early = [at(0, "o"), at(0, "x")]
        for k in range(1, last):
            early += [at(s, side) for s in (k, -k) for side in ("o", "x")]

        def early_tile(n, c):
            cols = pl.ds(pl.multiple_of(n * tile, tile), tile)
            acc[:, cols] = gather_dot(early, cols)
            return c

        lax.fori_loop(0, tiles, early_tile, 0)

    up_forward("o", last)
    down_forward(last)
    up_forward("x", last)

    def late_tile(n, c):
        cols = pl.ds(pl.multiple_of(n * tile, tile), tile)
        if streaming:
            lifted = acc[:, cols] + gather_dot([at(last, "o"), at(last, "x")], cols)
        else:
            lifted = jnp.dot(normed[...], up_all[:, cols], preferred_element_type=F32)
        lifted = jnp.maximum(lifted, 0.0)
        act[:, cols] = (lifted * lifted).astype(BF16)
        return c

    lax.fori_loop(0, tiles, late_tile, 0)

    def lower(start, size):
        cols = pl.ds(pl.multiple_of(start, size), size)
        fin[:, cols] = lax.dot_general(
            act[...], down_all[cols, :], (((1,), (1,)), ((), ())), preferred_element_type=F32
        ).astype(BF16)
        for d in range(1, n_tp):
            peer = lax.rem(tp + d, n_tp)
            pltpu.make_async_remote_copy(
                src_ref=fin.at[pl.ds(pl.multiple_of(peer * own, own), own), cols],
                dst_ref=fin_in.at[tp, :, cols],
                send_sem=tsend.at[2, d], recv_sem=trecv.at[2, d],
                device_id=(me, peer), device_id_type=MESH,
            ).start()

    def take(key):
        started[key].wait_recv()

    if streaming:
        lower(me * piece, piece)
        for k in range(1, last):
            for sign in (1, -1):
                lower(at(-sign * k, "o") * piece, piece)
        lower(at(last, "o") * piece, piece)
        take(down_x_key)
        lower(beside * piece, piece)
        for k in range(1, last):
            for sign in (1, -1):
                take(("f", k, sign))
                lower(at(-sign * k, "x") * piece, piece)
        for sign in (1, -1):
            take(("f", last, sign))
        lower(at(last, "x") * piece, piece)
    else:
        take(down_x_key)
        for k in range(1, last + 1):
            for sign in (1, -1):
                take(("f", k, sign))

        def block(b, c):
            lower(b * 256, 256)
            return c

        lax.fori_loop(0, width // 256, block, 0)

    for d in range(1, n_tp):
        peer = lax.rem(tp + d, n_tp)
        whole = pltpu.make_async_remote_copy(
            src_ref=fin.at[pl.ds(pl.multiple_of(peer * own, own), own), :],
            dst_ref=fin_in.at[lax.rem(tp - d + n_tp, n_tp)],
            send_sem=tsend.at[2, d], recv_sem=trecv.at[2, d],
            device_id=(me, peer), device_id_type=MESH,
        )
        whole.wait_recv()
        whole.wait_send()

    def finish(r, c):
        here = pl.ds(pl.multiple_of(r * slab, slab), slab)
        there = pl.ds(pl.multiple_of(tp * own + r * slab, slab), slab)
        total = fin[there, :].astype(F32)
        for d in range(1, n_tp):
            total = total + fin_in[lax.rem(tp + d, n_tp), here, :].astype(F32)
        out_ref[here, :] = (upd[here, :].astype(F32) + total).astype(BF16)
        return c

    lax.fori_loop(0, own // slab, finish, 0)
    for copy in list(started.values()) + carries + sums + shares:
        copy.wait_send()


def copy_ids(n_sp):
    last = n_sp // 4
    keys = [("ux",), ("dx",), ("halo",)]
    for k in range(1, last + 1):
        for sign in (1, -1):
            keys += [("u", "o", k, sign), ("u", "x", k, sign), ("d", "o", k, sign), ("f", k, sign)]
    return {key: n for n, key in enumerate(keys)}


def solution(mesh):
    n_sp, n_tp = mesh.shape["sp"], mesh.shape["tp"]
    ids = copy_ids(n_sp)

    def local(res, gate, value, conv, rate, inp, decay, step, outw, gain, up, down):
        rows, ch = value.shape
        width, hidden = outw.shape[1], up.shape[1]
        own = rows // n_tp
        V = pltpu.VMEM
        any_spec = pl.BlockSpec(memory_space=pl.ANY)
        vm = pl.BlockSpec(memory_space=pltpu.VMEM)
        dma = pltpu.SemaphoreType.DMA
        return pl.pallas_call(
            functools.partial(kernel, (n_sp, n_tp, ids)),
            out_shape=jax.ShapeDtypeStruct((own, width), BF16),
            in_specs=[any_spec, any_spec, any_spec, vm, vm, vm, vm, any_spec, any_spec, vm,
                      any_spec, any_spec],
            out_specs=vm,
            scratch_shapes=[
                V((width, hidden), BF16), V((width, hidden), BF16),
                V((rows, hidden), F32), V((rows, hidden), BF16), V((rows, width), BF16),
                V((rows, width), BF16), V((n_tp, own, width), BF16),
                V((rows, width), BF16), V((n_tp, own, width), BF16),
                V((ch // 128, rows, 128), F32), V((ch // 128, rows, 128), F32), V((rows + 8, ch), F32),
                V((rows, ch), BF16), V((rows, ch), BF16), V((rows, ch), BF16),
                V((rows, ch), F32), V((ch, width), BF16), V((own, width), BF16),
                V((16, ch), BF16), V((n_sp, 8, ch), F32), V((SCAN, 8, ch), F32),
                V((own, width), BF16), V((2, ch // 128, 128, 128), BF16),
                dma((len(ids),)), dma((len(ids),)), dma((3, n_tp)), dma((3, n_tp)),
                dma((n_sp,)), dma((n_sp,)), dma((7,)),
            ],
            compiler_params=pltpu.CompilerParams(
                collective_id=0, has_side_effects=True, vmem_limit_bytes=62 * 1024 * 1024
            ),
        )(res, gate, value, conv, rate, inp, decay.reshape(1, -1), step, outw,
          gain.reshape(1, -1), up, down)

    in_specs = (
        P("sp", None), P("sp", "tp"), P("sp", "tp"), P(None, "tp"),
        P("tp", None, None), P("tp", None, None), P("tp"), P("sp", "tp"),
        P("tp", None), P(), P("sp", "tp"), P("sp", "tp"),
    )
    return jax.shard_map(
        local, mesh=mesh, in_specs=in_specs, out_specs=P(("sp", "tp"), None), check_vma=False
    )
```

```python
import functools

import jax
import jax.numpy as jnp
from jax import lax
from jax.experimental import pallas as pl
from jax.experimental.pallas import tpu as pltpu
from jax.sharding import PartitionSpec as P

MESH = pl.DeviceIdType.MESH
F32 = jnp.float32
BF16 = jnp.bfloat16
SCAN = 8


def one_minus_exp(y):
    series = 1.0 + y * (1.0 / 7.0)
    for n in (6.0, 5.0, 4.0, 3.0, 2.0):
        series = 1.0 + y * (1.0 / n) * series
    return jnp.where(y > -0.3, -y * series, 1.0 - jnp.exp(y))


def kernel(
    dims,
    res_hbm, gate_hbm, value_hbm, conv_ref, rate_ref, inp_ref, decay_ref, step_hbm,
    outw_hbm, gain_ref, up_hbm, down_hbm,
    out_ref,
    up_all, down_all, act, normed, part, part_in, fin, fin_in,
    keep, drive, pad, gated, gate_v, value_v, step_v, outw_v, res_v, halo, tot, ent,
    upd, wpair, send, recv, tsend, trecv, csend, crecv, local_sem,
):
    n_sp, n_tp, ids = dims
    me, tp = lax.axis_index("sp"), lax.axis_index("tp")
    high = n_sp // 2
    hi, lo = me // 2, lax.rem(me, 2)
    rows, ch = value_v.shape
    width = up_all.shape[0]
    hidden = up_all.shape[1]
    piece = up_hbm.shape[0]
    own = rows // n_tp

    def at(step, side):
        low = lo if side == "o" else 1 - lo
        return lax.rem(hi + step + 2 * high, high) * 2 + low

    beside, above, below = at(0, "x"), at(1, "o"), at(-1, "o")

    loads = {}
    for n, (key, src, dst) in enumerate(
        (
            ("value", value_hbm, value_v),
            ("step", step_hbm, step_v),
            ("gate", gate_hbm, gate_v),
            ("outw", outw_hbm, outw_v),
            ("res", res_hbm.at[pl.ds(pl.multiple_of(tp * own, own), own), :], res_v),
            ("up", up_hbm, up_all.at[pl.ds(pl.multiple_of(me * piece, piece), piece), :]),
            ("down", down_hbm, down_all.at[pl.ds(pl.multiple_of(me * piece, piece), piece), :]),
        )
    ):
        loads[key] = pltpu.make_async_copy(src, dst, local_sem.at[n])
        loads[key].start()

    barrier = pltpu.get_barrier_semaphore()
    for d in range(1, n_sp):
        pl.semaphore_signal(
            barrier, inc=1, device_id=(lax.rem(me + d, n_sp), tp), device_id_type=MESH
        )
    for d in range(1, n_tp):
        pl.semaphore_signal(
            barrier, inc=1, device_id=(me, lax.rem(tp + d, n_tp)), device_id_type=MESH
        )
    pl.semaphore_wait(barrier, n_sp + n_tp - 2)

    started = {}

    def guarded(cond, act_on):
        if cond is None:
            act_on()
        else:
            pl.when(cond)(act_on)

    def launch(key, src, dst, target, send_if=None, recv_if=None):
        copy = pltpu.make_async_remote_copy(
            src_ref=src, dst_ref=dst, send_sem=send.at[ids[key]], recv_sem=recv.at[ids[key]],
            device_id=target, device_id_type=MESH,
        )
        guarded(send_if, copy.start)
        started[key] = (copy, send_if, recv_if)

    def take(key):
        copy, _, recv_if = started[key]
        guarded(recv_if, copy.wait_recv)

    split = max(16, piece * 3 // 8 // 16 * 16)
    streams = {
        "a": (up_hbm, 0, split, up_all),
        "b": (up_hbm, split, piece - split, up_all),
        "c": (down_hbm, 0, piece, down_all),
    }

    def landed(name, source):
        _, start, size, buf = streams[name]
        return buf.at[pl.ds(pl.multiple_of(source * piece + start, 16), size), :]

    def origin(name):
        hbm, start, size, _ = streams[name]
        return hbm.at[pl.ds(start, size), :]

    def has(k, sign):
        return hi >= k if sign > 0 else hi + k < high

    def line(name, side, k):
        for sign in (1, -1):
            source = at(-sign * (k - 1), side)
            dst = landed(name, source)
            src = origin(name) if k == 1 and side == "o" else dst
            onward = hi + 1 < high if sign > 0 else hi >= 1
            send_if = onward if k == 1 else jnp.logical_and(onward, has(k - 1, sign))
            launch((name, side, k, sign), src, dst, (above if sign > 0 else below, tp),
                   send_if, has(k, sign))

    def across(name):
        launch((name, "x"), origin(name), landed(name, me), (beside, tp))

    def forward(name, side, k):
        for sign in (1, -1):
            take((name, side, k, sign))
        if k < high - 1:
            line(name, side, k + 1)
        if name != "a":
            for sign in (1, -1):
                view = landed(name, at(-sign * k, "o"))
                launch((name, "f", k, sign), view, view, (beside, tp), has(k, sign), has(k, sign))

    halo_copy_key = ("halo",)
    launch(
        halo_copy_key, value_hbm.at[pl.ds(rows - 16, 16), :], halo,
        (lax.rem(me + 1, n_sp), tp),
    )
    line("a", "o", 1)
    line("b", "o", 1)
    across("a")
    across("b")

    bw = rate_ref.shape[1]
    per = 128 // bw
    groups = ch // 128
    r_i = lax.broadcasted_iota(jnp.int32, (bw, 128), 0)
    c_i = lax.broadcasted_iota(jnp.int32, (bw, 128), 1)
    for g in range(groups):
        for which, ref in ((0, rate_ref), (1, inp_ref)):
            for j in range(per):
                place = jnp.where(c_i == r_i + j * bw, 1.0, 0.0).astype(BF16)
                block = jnp.dot(ref[g * per + j], place, preferred_element_type=F32)
                wpair[which, g, j * bw : (j + 1) * bw, :] = block.astype(BF16)

    loads["value"].wait()
    loads["step"].wait()
    take(halo_copy_key)
    taps = conv_ref.shape[0]
    first = jnp.where(me == 0, 0.0, 1.0).astype(F32)
    pad[0:8, :] = halo[8:16, :].astype(F32) * first

    chunk = 64

    def widen(r, c):
        at_row = pl.multiple_of(r * chunk, chunk)
        pad[pl.ds(pl.multiple_of(at_row + 8, 8), chunk), :] = value_v[
            pl.ds(at_row, chunk), :
        ].astype(F32)
        return c

    lax.fori_loop(0, rows // chunk, widen, 0)

    def gates(r, c):
        at_row = pl.multiple_of(r * chunk, chunk)
        for g in range(groups):
            lanes = slice(g * 128, (g + 1) * 128)
            window = pad[pl.ds(at_row, chunk + 8), lanes]
            total = jnp.zeros((chunk, 128), F32)
            for k in range(taps):
                shift = 8 - taps + 1 + k
                moved = window if shift == 0 else pltpu.roll(window, chunk + 8 - shift, 0)
                total = total + moved[0:chunk, :] * conv_ref[k : k + 1, lanes]
            smooth = total.astype(BF16)
            rate = lax.logistic(jnp.dot(smooth, wpair[0, g], preferred_element_type=F32))
            gate = lax.logistic(jnp.dot(smooth, wpair[1, g], preferred_element_type=F32))
            log_keep = -8.0 * step_v[pl.ds(at_row, chunk), lanes] * rate * decay_ref[0:1, lanes]
            keep[g, pl.ds(at_row, chunk), :] = jnp.exp(log_keep)
            drive[g, pl.ds(at_row, chunk), :] = (
                jnp.sqrt(one_minus_exp(2.0 * log_keep)) * gate * smooth.astype(F32)
            )
        return c

    lax.fori_loop(0, rows // chunk, gates, 0)

    seg = rows // SCAN

    def scan(i, carry):
        p, h = carry
        idx = pl.ds(i, SCAN, stride=seg)
        new_p, new_h = [], []
        for g in range(groups):
            a, d = keep[g, idx, :], drive[g, idx, :]
            hg = a * h[g] + d
            pg = a * p[g]
            keep[g, idx, :] = pg
            drive[g, idx, :] = hg
            new_p.append(pg)
            new_h.append(hg)
        return tuple(new_p), tuple(new_h)

    ones = tuple(jnp.ones((SCAN, 128), F32) for _ in range(groups))
    zeros = tuple(jnp.zeros((SCAN, 128), F32) for _ in range(groups))
    lax.fori_loop(0, seg, scan, (ones, zeros))

    def pick(ref, row):
        return jnp.concatenate([ref[g, row : row + 1, :] for g in range(groups)], axis=1)

    ends = [(pick(keep, (b + 1) * seg - 1), pick(drive, (b + 1) * seg - 1)) for b in range(SCAN)]
    whole_p, whole_h = ends[0]
    for p_b, h_b in ends[1:]:
        whole_p, whole_h = whole_p * p_b, p_b * whole_h + h_b
    row_id = lax.broadcasted_iota(jnp.int32, (8, ch), 0)
    tot[me] = jnp.where(row_id == 0, whole_p, whole_h)
    carries = []
    for d in range(1, n_sp):
        copy = pltpu.make_async_remote_copy(
            src_ref=tot.at[me], dst_ref=tot.at[me], send_sem=csend.at[d], recv_sem=crecv.at[d],
            device_id=(lax.rem(me + d, n_sp), tp), device_id_type=MESH,
        )
        copy.start()
        carries.append(copy)
    loads["gate"].wait()
    loads["outw"].wait()
    for copy in carries:
        copy.wait_recv()

    def fold(d, s):
        joined = tot[d, 0:1, :] * s + tot[d, 1:2, :]
        return jnp.where(d < me, joined, s)

    state = lax.fori_loop(0, n_sp, fold, jnp.zeros((1, ch), F32))
    for b in range(SCAN):
        ent[b, 0:1, :] = state
        state = ends[b][0] * state + ends[b][1]

    def gating(b, c):
        at_row = pl.ds(pl.multiple_of(b * seg, seg), seg)
        for g in range(groups):
            lanes = slice(g * 128, (g + 1) * 128)
            full = drive[g, at_row, :] + keep[g, at_row, :] * ent[b, 0:1, lanes]
            branch = jax.nn.gelu(gate_v[at_row, lanes].astype(F32), approximate=True)
            gated[at_row, lanes] = (branch * full).astype(BF16)
        return c

    lax.fori_loop(0, SCAN, gating, 0)

    sums = []
    for d in list(range(1, n_tp)) + [0]:
        peer = lax.rem(tp + d, n_tp)
        span = pl.ds(pl.multiple_of(peer * own, own), own)
        part[span, :] = jnp.dot(gated[span, :], outw_v[...], preferred_element_type=F32).astype(BF16)
        if d:
            copy = pltpu.make_async_remote_copy(
                src_ref=part.at[span, :], dst_ref=part_in.at[tp],
                send_sem=tsend.at[0, d], recv_sem=trecv.at[0, d],
                device_id=(me, peer), device_id_type=MESH,
            )
            copy.start()
            sums.append(copy)

    forward("a", "o", 1)
    forward("b", "o", 1)
    take(("a", "x"))
    line("a", "x", 1)
    line("c", "o", 1)
    across("c")

    mine = pl.ds(pl.multiple_of(tp * own, own), own)
    loads["res"].wait()
    for copy in sums:
        copy.wait_recv()
    slab = 32

    def settle(r, c):
        here = pl.ds(pl.multiple_of(r * slab, slab), slab)
        there = pl.ds(pl.multiple_of(tp * own + r * slab, slab), slab)
        mixed = part[there, :].astype(F32)
        for d in range(1, n_tp):
            mixed = mixed + part_in[lax.rem(tp + d, n_tp), here, :].astype(F32)
        new = (res_v[here, :].astype(F32) + mixed).astype(BF16)
        upd[here, :] = new
        wide = new.astype(F32)
        factor = lax.rsqrt(jnp.mean(wide * wide, axis=-1, keepdims=True) + 1e-06)
        normed[there, :] = (wide * factor * gain_ref[0:1, :]).astype(BF16)
        return c

    lax.fori_loop(0, own // slab, settle, 0)
    shares = []
    for d in range(1, n_tp):
        copy = pltpu.make_async_remote_copy(
            src_ref=normed.at[mine, :], dst_ref=normed.at[mine, :],
            send_sem=tsend.at[1, d], recv_sem=trecv.at[1, d],
            device_id=(me, lax.rem(tp + d, n_tp)), device_id_type=MESH,
        )
        copy.start()
        shares.append(copy)

    for k in range(2, high):
        forward("b", "o", k)
        forward("a", "o", k)
        forward("a", "x", k - 1)
        forward("c", "o", k - 1)
    forward("a", "x", high - 1)
    for copy in shares:
        copy.wait_recv()
    loads["up"].wait()
    loads["down"].wait()

    streaming = piece % 128 == 0
    tile = 512
    tiles = hidden // tile

    take(("b", "x"))
    for k in range(1, high):
        for sign in (1, -1):
            take(("b", "f", k, sign))

    def late_tile(n, c):
        cols = pl.ds(pl.multiple_of(n * tile, tile), tile)
        lifted = jnp.dot(normed[...], up_all[:, cols], preferred_element_type=F32)
        lifted = jnp.maximum(lifted, 0.0)
        act[:, cols] = (lifted * lifted).astype(BF16)
        return c

    lax.fori_loop(0, tiles, late_tile, 0)

    def lower(start, size):
        cols = pl.ds(pl.multiple_of(start, size), size)
        fin[:, cols] = lax.dot_general(
            act[...], down_all[cols, :], (((1,), (1,)), ((), ())), preferred_element_type=F32
        ).astype(BF16)
        for d in range(1, n_tp):
            peer = lax.rem(tp + d, n_tp)
            pltpu.make_async_remote_copy(
                src_ref=fin.at[pl.ds(pl.multiple_of(peer * own, own), own), cols],
                dst_ref=fin_in.at[tp, :, cols],
                send_sem=tsend.at[2, d], recv_sem=trecv.at[2, d],
                device_id=(me, peer), device_id_type=MESH,
            ).start()

    if streaming:
        def lower_if(k, sign, side):
            pl.when(has(k, sign))(lambda: lower(at(-sign * k, side) * piece, piece))

        lower(me * piece, piece)
        for k in range(1, high):
            if k == high - 1:
                forward("c", "o", k)
            for sign in (1, -1):
                lower_if(k, sign, "o")
        take(("c", "x"))
        lower(beside * piece, piece)
        for k in range(1, high):
            for sign in (1, -1):
                take(("c", "f", k, sign))
                lower_if(k, sign, "x")
    else:
        forward("c", "o", high - 1)
        take(("c", "x"))
        for k in range(1, high):
            for sign in (1, -1):
                take(("c", "f", k, sign))

        def block(b, c):
            lower(b * 256, 256)
            return c

        lax.fori_loop(0, width // 256, block, 0)

    for d in range(1, n_tp):
        peer = lax.rem(tp + d, n_tp)
        whole = pltpu.make_async_remote_copy(
            src_ref=fin.at[pl.ds(pl.multiple_of(peer * own, own), own), :],
            dst_ref=fin_in.at[lax.rem(tp - d + n_tp, n_tp)],
            send_sem=tsend.at[2, d], recv_sem=trecv.at[2, d],
            device_id=(me, peer), device_id_type=MESH,
        )
        whole.wait_recv()
        whole.wait_send()

    def finish(r, c):
        here = pl.ds(pl.multiple_of(r * slab, slab), slab)
        there = pl.ds(pl.multiple_of(tp * own + r * slab, slab), slab)
        total = fin[there, :].astype(F32)
        for d in range(1, n_tp):
            total = total + fin_in[lax.rem(tp + d, n_tp), here, :].astype(F32)
        out_ref[here, :] = (upd[here, :].astype(F32) + total).astype(BF16)
        return c

    lax.fori_loop(0, own // slab, finish, 0)
    for copy, send_if, _ in started.values():
        guarded(send_if, copy.wait_send)
    for copy in carries + sums + shares:
        copy.wait_send()


def copy_ids(n_sp):
    keys = [("a", "x"), ("b", "x"), ("c", "x"), ("halo",)]
    for k in range(1, n_sp // 2):
        for sign in (1, -1):
            keys += [(name, side, k, sign) for name, side in
                     (("a", "o"), ("a", "x"), ("b", "o"), ("c", "o"), ("b", "f"), ("c", "f"))]
    return {key: n for n, key in enumerate(keys)}


def solution(mesh):
    n_sp, n_tp = mesh.shape["sp"], mesh.shape["tp"]
    ids = copy_ids(n_sp)

    def local(res, gate, value, conv, rate, inp, decay, step, outw, gain, up, down):
        rows, ch = value.shape
        width, hidden = outw.shape[1], up.shape[1]
        own = rows // n_tp
        V = pltpu.VMEM
        any_spec = pl.BlockSpec(memory_space=pl.ANY)
        vm = pl.BlockSpec(memory_space=pltpu.VMEM)
        dma = pltpu.SemaphoreType.DMA
        return pl.pallas_call(
            functools.partial(kernel, (n_sp, n_tp, ids)),
            out_shape=jax.ShapeDtypeStruct((own, width), BF16),
            in_specs=[any_spec, any_spec, any_spec, vm, vm, vm, vm, any_spec, any_spec, vm,
                      any_spec, any_spec],
            out_specs=vm,
            scratch_shapes=[
                V((width, hidden), BF16), V((width, hidden), BF16),
                V((rows, hidden), BF16), V((rows, width), BF16),
                V((rows, width), BF16), V((n_tp, own, width), BF16),
                V((rows, width), BF16), V((n_tp, own, width), BF16),
                V((ch // 128, rows, 128), F32), V((ch // 128, rows, 128), F32), V((rows + 8, ch), F32),
                V((rows, ch), BF16), V((rows, ch), BF16), V((rows, ch), BF16),
                V((rows, ch), F32), V((ch, width), BF16), V((own, width), BF16),
                V((16, ch), BF16), V((n_sp, 8, ch), F32), V((SCAN, 8, ch), F32),
                V((own, width), BF16), V((2, ch // 128, 128, 128), BF16),
                dma((len(ids),)), dma((len(ids),)), dma((3, n_tp)), dma((3, n_tp)),
                dma((n_sp,)), dma((n_sp,)), dma((7,)),
            ],
            compiler_params=pltpu.CompilerParams(
                collective_id=0, has_side_effects=True, vmem_limit_bytes=62 * 1024 * 1024
            ),
        )(res, gate, value, conv, rate, inp, decay.reshape(1, -1), step, outw,
          gain.reshape(1, -1), up, down)

    in_specs = (
        P("sp", None), P("sp", "tp"), P("sp", "tp"), P(None, "tp"),
        P("tp", None, None), P("tp", None, None), P("tp"), P("sp", "tp"),
        P("tp", None), P(), P("sp", "tp"), P("sp", "tp"),
    )
    return jax.shard_map(
        local, mesh=mesh, in_specs=in_specs, out_specs=P(("sp", "tp"), None), check_vma=False
    )
```

```python
import functools

import jax
import jax.numpy as jnp
from jax import lax
from jax.experimental import pallas as pl
from jax.experimental.pallas import tpu as pltpu
from jax.sharding import PartitionSpec as P

MESH = pl.DeviceIdType.MESH
F32 = jnp.float32
BF16 = jnp.bfloat16
SCAN = 8


def one_minus_exp(y):
    series = 1.0 + y * (1.0 / 7.0)
    for n in (6.0, 5.0, 4.0, 3.0, 2.0):
        series = 1.0 + y * (1.0 / n) * series
    return jnp.where(y > -0.3, -y * series, 1.0 - jnp.exp(y))


def kernel(
    dims,
    res_hbm, gate_hbm, value_hbm, conv_ref, rate_ref, inp_ref, decay_ref, step_hbm,
    outw_hbm, gain_ref, up_hbm, down_hbm,
    out_ref,
    up_all, down_all, act, normed, part, part_in, fin, fin_in, far_out, far_in,
    keep, drive, pad, gated, gate_v, value_v, step_v, outw_v, res_v, halo, tot, ent,
    upd, wpair, send, recv, tsend, trecv, fsend, frecv, csend, crecv, local_sem,
):
    n_sp, n_tp, ids = dims
    me, tp = lax.axis_index("sp"), lax.axis_index("tp")
    half_size = n_sp // 2
    high = half_size // 2
    half, place_in = me // half_size, lax.rem(me, half_size)
    hi, lo = place_in // 2, lax.rem(place_in, 2)
    partner = lax.rem(me + half_size, n_sp)
    rows, ch = value_v.shape
    width = up_all.shape[0]
    hidden = up_all.shape[1]
    piece = up_hbm.shape[0]
    own = rows // n_tp

    def at(step, side):
        low = lo if side == "o" else 1 - lo
        return half * half_size + lax.rem(hi + step + 2 * high, high) * 2 + low

    beside, above, below = at(0, "x"), at(1, "o"), at(-1, "o")

    kept = pl.ds(pl.multiple_of(half * hidden, 128), hidden)
    given = pl.ds(pl.multiple_of((1 - half) * hidden, 128), hidden)

    loads = {}
    for n, (key, src, dst) in enumerate(
        (
            ("value", value_hbm, value_v),
            ("step", step_hbm, step_v),
            ("gate", gate_hbm, gate_v),
            ("outw", outw_hbm, outw_v),
            ("res", res_hbm.at[pl.ds(pl.multiple_of(tp * own, own), own), :], res_v),
            ("up", up_hbm.at[:, kept], up_all.at[pl.ds(pl.multiple_of(me * piece, piece), piece), :]),
            ("down", down_hbm.at[:, kept], down_all.at[pl.ds(pl.multiple_of(me * piece, piece), piece), :]),
        )
    ):
        loads[key] = pltpu.make_async_copy(src, dst, local_sem.at[n])
        loads[key].start()

    barrier = pltpu.get_barrier_semaphore()
    for d in range(1, n_sp):
        pl.semaphore_signal(
            barrier, inc=1, device_id=(lax.rem(me + d, n_sp), tp), device_id_type=MESH
        )
    for d in range(1, n_tp):
        pl.semaphore_signal(
            barrier, inc=1, device_id=(me, lax.rem(tp + d, n_tp)), device_id_type=MESH
        )
    pl.semaphore_wait(barrier, n_sp + n_tp - 2)

    started = {}

    def guarded(cond, act_on):
        if cond is None:
            act_on()
        else:
            pl.when(cond)(act_on)

    def launch(key, src, dst, target, send_if=None, recv_if=None):
        copy = pltpu.make_async_remote_copy(
            src_ref=src, dst_ref=dst, send_sem=send.at[ids[key]], recv_sem=recv.at[ids[key]],
            device_id=target, device_id_type=MESH,
        )
        guarded(send_if, copy.start)
        started[key] = (copy, send_if, recv_if)

    def take(key):
        copy, _, recv_if = started[key]
        guarded(recv_if, copy.wait_recv)

    streams = {
        "u": (up_hbm, False, up_all),
        "v": (up_hbm, True, up_all),
        "c": (down_hbm, False, down_all),
        "e": (down_hbm, True, down_all),
    }

    def landed(name, source):
        _, far, buf = streams[name]
        if far:
            source = lax.rem(source + half_size, n_sp)
        return buf.at[pl.ds(pl.multiple_of(source * piece, 16), piece), :]

    def origin(name):
        hbm, far, _ = streams[name]
        return landed(name, me) if far else hbm.at[:, kept]

    def has(k, sign):
        return hi >= k if sign > 0 else hi + k < high

    def line(name, k):
        for sign in (1, -1):
            dst = landed(name, at(-sign * (k - 1), "o"))
            src = origin(name) if k == 1 else dst
            onward = hi + 1 < high if sign > 0 else hi >= 1
            send_if = onward if k == 1 else jnp.logical_and(onward, has(k - 1, sign))
            launch((name, "o", k, sign), src, dst, (above if sign > 0 else below, tp),
                   send_if, has(k, sign))

    def across(name):
        launch((name, "x"), origin(name), landed(name, me), (beside, tp))

    def forward(name, k):
        for sign in (1, -1):
            take((name, "o", k, sign))
        if k < high - 1:
            line(name, k + 1)
        for sign in (1, -1):
            view = landed(name, at(-sign * k, "o"))
            launch((name, "f", k, sign), view, view, (beside, tp), has(k, sign), has(k, sign))

    halo_copy_key = ("halo",)
    launch(
        halo_copy_key, value_hbm.at[pl.ds(rows - 16, 16), :], halo,
        (lax.rem(me + 1, n_sp), tp),
    )
    mine_up = up_all.at[pl.ds(pl.multiple_of(me * piece, 16), piece), :]
    mine_down = down_all.at[pl.ds(pl.multiple_of(me * piece, 16), piece), :]
    launch(("pu",), up_hbm.at[:, given], mine_up, (partner, tp))
    line("u", 1)
    across("u")
    launch(("pd",), down_hbm.at[:, given], mine_down, (partner, tp))
    line("c", 1)
    across("c")

    bw = rate_ref.shape[1]
    per = 128 // bw
    groups = ch // 128
    r_i = lax.broadcasted_iota(jnp.int32, (bw, 128), 0)
    c_i = lax.broadcasted_iota(jnp.int32, (bw, 128), 1)
    for g in range(groups):
        for which, ref in ((0, rate_ref), (1, inp_ref)):
            for j in range(per):
                place = jnp.where(c_i == r_i + j * bw, 1.0, 0.0).astype(BF16)
                block = jnp.dot(ref[g * per + j], place, preferred_element_type=F32)
                wpair[which, g, j * bw : (j + 1) * bw, :] = block.astype(BF16)

    loads["value"].wait()
    loads["step"].wait()
    take(halo_copy_key)
    taps = conv_ref.shape[0]
    first = jnp.where(me == 0, 0.0, 1.0).astype(F32)
    pad[0:8, :] = halo[8:16, :].astype(F32) * first

    chunk = 64

    def widen(r, c):
        at_row = pl.multiple_of(r * chunk, chunk)
        pad[pl.ds(pl.multiple_of(at_row + 8, 8), chunk), :] = value_v[
            pl.ds(at_row, chunk), :
        ].astype(F32)
        return c

    lax.fori_loop(0, rows // chunk, widen, 0)

    def gates(r, c):
        at_row = pl.multiple_of(r * chunk, chunk)
        for g in range(groups):
            lanes = slice(g * 128, (g + 1) * 128)
            window = pad[pl.ds(at_row, chunk + 8), lanes]
            total = jnp.zeros((chunk, 128), F32)
            for k in range(taps):
                shift = 8 - taps + 1 + k
                moved = window if shift == 0 else pltpu.roll(window, chunk + 8 - shift, 0)
                total = total + moved[0:chunk, :] * conv_ref[k : k + 1, lanes]
            smooth = total.astype(BF16)
            rate = lax.logistic(jnp.dot(smooth, wpair[0, g], preferred_element_type=F32))
            gate = lax.logistic(jnp.dot(smooth, wpair[1, g], preferred_element_type=F32))
            log_keep = -8.0 * step_v[pl.ds(at_row, chunk), lanes] * rate * decay_ref[0:1, lanes]
            keep[g, pl.ds(at_row, chunk), :] = jnp.exp(log_keep)
            drive[g, pl.ds(at_row, chunk), :] = (
                jnp.sqrt(one_minus_exp(2.0 * log_keep)) * gate * smooth.astype(F32)
            )
        return c

    lax.fori_loop(0, rows // chunk, gates, 0)

    seg = rows // SCAN

    def scan(i, carry):
        p, h = carry
        idx = pl.ds(i, SCAN, stride=seg)
        new_p, new_h = [], []
        for g in range(groups):
            a, d = keep[g, idx, :], drive[g, idx, :]
            hg = a * h[g] + d
            pg = a * p[g]
            keep[g, idx, :] = pg
            drive[g, idx, :] = hg
            new_p.append(pg)
            new_h.append(hg)
        return tuple(new_p), tuple(new_h)

    ones = tuple(jnp.ones((SCAN, 128), F32) for _ in range(groups))
    zeros = tuple(jnp.zeros((SCAN, 128), F32) for _ in range(groups))
    lax.fori_loop(0, seg, scan, (ones, zeros))

    def pick(ref, row):
        return jnp.concatenate([ref[g, row : row + 1, :] for g in range(groups)], axis=1)

    ends = [(pick(keep, (b + 1) * seg - 1), pick(drive, (b + 1) * seg - 1)) for b in range(SCAN)]
    whole_p, whole_h = ends[0]
    for p_b, h_b in ends[1:]:
        whole_p, whole_h = whole_p * p_b, p_b * whole_h + h_b
    row_id = lax.broadcasted_iota(jnp.int32, (8, ch), 0)
    tot[me] = jnp.where(row_id == 0, whole_p, whole_h)
    carries = []
    for d in range(1, n_sp):
        copy = pltpu.make_async_remote_copy(
            src_ref=tot.at[me], dst_ref=tot.at[me], send_sem=csend.at[d], recv_sem=crecv.at[d],
            device_id=(lax.rem(me + d, n_sp), tp), device_id_type=MESH,
        )
        copy.start()
        carries.append(copy)
    loads["gate"].wait()
    loads["outw"].wait()
    for copy in carries:
        copy.wait_recv()

    def fold(d, s):
        joined = tot[d, 0:1, :] * s + tot[d, 1:2, :]
        return jnp.where(d < me, joined, s)

    state = lax.fori_loop(0, n_sp, fold, jnp.zeros((1, ch), F32))
    for b in range(SCAN):
        ent[b, 0:1, :] = state
        state = ends[b][0] * state + ends[b][1]

    def gating(b, c):
        at_row = pl.ds(pl.multiple_of(b * seg, seg), seg)
        for g in range(groups):
            lanes = slice(g * 128, (g + 1) * 128)
            full = drive[g, at_row, :] + keep[g, at_row, :] * ent[b, 0:1, lanes]
            branch = jax.nn.gelu(gate_v[at_row, lanes].astype(F32), approximate=True)
            gated[at_row, lanes] = (branch * full).astype(BF16)
        return c

    lax.fori_loop(0, SCAN, gating, 0)

    sums = []
    for d in list(range(1, n_tp)) + [0]:
        peer = lax.rem(tp + d, n_tp)
        span = pl.ds(pl.multiple_of(peer * own, own), own)
        part[span, :] = jnp.dot(gated[span, :], outw_v[...], preferred_element_type=F32).astype(BF16)
        if d:
            copy = pltpu.make_async_remote_copy(
                src_ref=part.at[span, :], dst_ref=part_in.at[tp],
                send_sem=tsend.at[0, d], recv_sem=trecv.at[0, d],
                device_id=(me, peer), device_id_type=MESH,
            )
            copy.start()
            sums.append(copy)

    take(("pu",))
    line("v", 1)
    across("v")
    forward("u", 1)

    mine = pl.ds(pl.multiple_of(tp * own, own), own)
    loads["res"].wait()
    for copy in sums:
        copy.wait_recv()
    slab = 32

    def settle(r, c):
        here = pl.ds(pl.multiple_of(r * slab, slab), slab)
        there = pl.ds(pl.multiple_of(tp * own + r * slab, slab), slab)
        mixed = part[there, :].astype(F32)
        for d in range(1, n_tp):
            mixed = mixed + part_in[lax.rem(tp + d, n_tp), here, :].astype(F32)
        new = (res_v[here, :].astype(F32) + mixed).astype(BF16)
        upd[here, :] = new
        wide = new.astype(F32)
        factor = lax.rsqrt(jnp.mean(wide * wide, axis=-1, keepdims=True) + 1e-06)
        normed[there, :] = (wide * factor * gain_ref[0:1, :]).astype(BF16)
        return c

    lax.fori_loop(0, own // slab, settle, 0)
    shares = []
    far_mine = pl.ds(pl.multiple_of(rows + tp * own, own), own)
    launch(("n",), normed.at[mine, :], normed.at[far_mine, :], (partner, tp))

    def share(span, turn):
        copies = []
        for d in range(1, n_tp):
            copy = pltpu.make_async_remote_copy(
                src_ref=normed.at[span, :], dst_ref=normed.at[span, :],
                send_sem=tsend.at[turn, d], recv_sem=trecv.at[turn, d],
                device_id=(me, lax.rem(tp + d, n_tp)), device_id_type=MESH,
            )
            copy.start()
            copies.append(copy)
        return copies

    shares = share(mine, 1)
    take(("pd",))
    line("e", 1)
    across("e")
    forward("c", 1)
    forward("v", 1)
    take(("n",))
    shares_far = share(far_mine, 2)
    forward("e", 1)
    for k in range(2, high):
        for name in ("u", "v", "c", "e"):
            forward(name, k)
    loads["up"].wait()
    loads["down"].wait()

    def settle_stream(name):
        take((name, "x"))
        for k in range(1, high):
            for sign in (1, -1):
                take((name, "f", k, sign))

    settle_stream("u")
    settle_stream("v")
    tile = 512

    for copy in shares:
        copy.wait_recv()
    def raise_rows(start):
        def one(n, c):
            cols = pl.ds(pl.multiple_of(n * tile, tile), tile)
            lifted = jnp.dot(
                normed[start : start + rows, :], up_all[:, cols], preferred_element_type=F32
            )
            lifted = jnp.maximum(lifted, 0.0)
            act[start : start + rows, cols] = (lifted * lifted).astype(BF16)
            return c

        lax.fori_loop(0, hidden // tile, one, 0)

    raise_rows(0)
    for copy in shares_far:
        copy.wait_recv()
    raise_rows(rows)
    settle_stream("c")
    settle_stream("e")
    blocks = width // tile
    lowered = {}

    def lower(side, q):
        cols = slice(q * tile, (q + 1) * tile)
        base = side * rows
        fin[base : base + rows, cols] = lax.dot_general(
            act[base : base + rows, :], down_all[cols, :], (((1,), (1,)), ((), ())),
            preferred_element_type=F32,
        ).astype(BF16)
        for d in range(1, n_tp):
            peer = lax.rem(tp + d, n_tp)
            copy = pltpu.make_async_remote_copy(
                src_ref=fin.at[pl.ds(pl.multiple_of(base + peer * own, own), own), cols],
                dst_ref=fin_in.at[tp, side * own : (side + 1) * own, cols],
                send_sem=fsend.at[side * blocks + q, d], recv_sem=frecv.at[side * blocks + q, d],
                device_id=(me, peer), device_id_type=MESH,
            )
            copy.start()
            lowered[side, q, d] = copy

    def gathered(side, r, cols):
        here = pl.ds(pl.multiple_of(side * own + r * slab, slab), slab)
        there = pl.ds(pl.multiple_of(side * rows + tp * own + r * slab, slab), slab)
        total = fin[there, cols].astype(F32)
        for d in range(1, n_tp):
            total = total + fin_in[lax.rem(tp + d, n_tp), here, cols].astype(F32)
        return total

    for side in (1, 0):
        for q in range(blocks):
            lower(side, q)
    for q in range(blocks):
        cols = slice(q * tile, (q + 1) * tile)
        for d in range(1, n_tp):
            lowered[1, q, d].wait_recv()

        def far_sum(r, c, cols=cols):
            here = pl.ds(pl.multiple_of(r * slab, slab), slab)
            far_out[here, cols] = gathered(1, r, cols).astype(BF16)
            return c

        lax.fori_loop(0, own // slab, far_sum, 0)
        launch(("r", q), far_out.at[:, cols], far_in.at[:, cols], (partner, tp))
    for q in range(blocks):
        cols = slice(q * tile, (q + 1) * tile)
        for d in range(1, n_tp):
            lowered[0, q, d].wait_recv()
        take(("r", q))

        def finish(r, c, cols=cols):
            here = pl.ds(pl.multiple_of(r * slab, slab), slab)
            total = gathered(0, r, cols) + far_in[here, cols].astype(F32)
            out_ref[here, cols] = (upd[here, cols].astype(F32) + total).astype(BF16)
            return c

        lax.fori_loop(0, own // slab, finish, 0)
    for copy, send_if, _ in started.values():
        guarded(send_if, copy.wait_send)
    for copy in carries + sums + shares + shares_far + list(lowered.values()):
        copy.wait_send()


def copy_ids(n_sp, blocks):
    keys = [("pu",), ("pd",), ("halo",), ("n",)] + [("r", q) for q in range(blocks)]
    for name in ("u", "v", "c", "e"):
        keys.append((name, "x"))
        for k in range(1, n_sp // 4):
            for sign in (1, -1):
                keys += [(name, "o", k, sign), (name, "f", k, sign)]
    return {key: n for n, key in enumerate(keys)}


def solution(mesh):
    n_sp, n_tp = mesh.shape["sp"], mesh.shape["tp"]

    def local(res, gate, value, conv, rate, inp, decay, step, outw, gain, up, down):
        rows, ch = value.shape
        width, hidden = outw.shape[1], up.shape[1]
        own = rows // n_tp
        hidden = hidden // 2
        ids = copy_ids(n_sp, width // 512)
        V = pltpu.VMEM
        any_spec = pl.BlockSpec(memory_space=pl.ANY)
        vm = pl.BlockSpec(memory_space=pltpu.VMEM)
        dma = pltpu.SemaphoreType.DMA
        return pl.pallas_call(
            functools.partial(kernel, (n_sp, n_tp, ids)),
            out_shape=jax.ShapeDtypeStruct((own, width), BF16),
            in_specs=[any_spec, any_spec, any_spec, vm, vm, vm, vm, any_spec, any_spec, vm,
                      any_spec, any_spec],
            out_specs=vm,
            scratch_shapes=[
                V((width, hidden), BF16), V((width, hidden), BF16),
                V((2 * rows, hidden), BF16), V((2 * rows, width), BF16),
                V((rows, width), BF16), V((n_tp, own, width), BF16),
                V((2 * rows, width), BF16), V((n_tp, 2 * own, width), BF16),
                V((own, width), BF16), V((own, width), BF16),
                V((ch // 128, rows, 128), F32), V((ch // 128, rows, 128), F32), V((rows + 8, ch), F32),
                V((rows, ch), BF16), V((rows, ch), BF16), V((rows, ch), BF16),
                V((rows, ch), F32), V((ch, width), BF16), V((own, width), BF16),
                V((16, ch), BF16), V((n_sp, 8, ch), F32), V((SCAN, 8, ch), F32),
                V((own, width), BF16), V((2, ch // 128, 128, 128), BF16),
                dma((len(ids),)), dma((len(ids),)), dma((3, n_tp)), dma((3, n_tp)),
                dma((2 * width // 512, n_tp)), dma((2 * width // 512, n_tp)),
                dma((n_sp,)), dma((n_sp,)), dma((7,)),
            ],
            compiler_params=pltpu.CompilerParams(
                collective_id=0, has_side_effects=True, vmem_limit_bytes=62 * 1024 * 1024
            ),
        )(res, gate, value, conv, rate, inp, decay.reshape(1, -1), step, outw,
          gain.reshape(1, -1), up, down)

    in_specs = (
        P("sp", None), P("sp", "tp"), P("sp", "tp"), P(None, "tp"),
        P("tp", None, None), P("tp", None, None), P("tp"), P("sp", "tp"),
        P("tp", None), P(), P("sp", "tp"), P("sp", "tp"),
    )
    return jax.shard_map(
        local, mesh=mesh, in_specs=in_specs, out_specs=P(("sp", "tp"), None), check_vma=False
    )
```

```python
import functools

import jax
import jax.numpy as jnp
from jax import lax
from jax.experimental import pallas as pl
from jax.experimental.pallas import tpu as pltpu
from jax.sharding import PartitionSpec as P

MESH = pl.DeviceIdType.MESH
F32 = jnp.float32
BF16 = jnp.bfloat16
SCAN = 8


def one_minus_exp(y):
    series = 1.0 + y * (1.0 / 7.0)
    for n in (6.0, 5.0, 4.0, 3.0, 2.0):
        series = 1.0 + y * (1.0 / n) * series
    return jnp.where(y > -0.3, -y * series, 1.0 - jnp.exp(y))


def kernel(
    dims,
    res_hbm, gate_hbm, value_hbm, conv_ref, rate_ref, inp_ref, decay_ref, step_hbm,
    outw_hbm, gain_ref, up_hbm, down_hbm,
    out_ref,
    up_all, down_all, act, normed, part, part_in, fin, fin_in, pair_in, far_out, far_in,
    keep, drive, pad, gated, gate_v, value_v, step_v, outw_v, res_v, halo, tot, ent,
    upd, wpair, send, recv, tsend, trecv, fsend, frecv, csend, crecv, local_sem,
):
    n_sp, n_tp, ids = dims
    me, tp = lax.axis_index("sp"), lax.axis_index("tp")
    half_size = n_sp // 2
    high = half_size // 2
    half, place_in = me // half_size, lax.rem(me, half_size)
    hi, lo = place_in // 2, lax.rem(place_in, 2)
    partner = lax.rem(me + half_size, n_sp)
    rows, ch = value_v.shape
    width = up_all.shape[0]
    hidden = up_all.shape[1]
    piece = up_hbm.shape[0]
    own = rows // n_tp

    def at(step, side):
        low = lo if side == "o" else 1 - lo
        return half * half_size + lax.rem(hi + step + 2 * high, high) * 2 + low

    beside, above, below = at(0, "x"), at(1, "o"), at(-1, "o")

    kept = pl.ds(pl.multiple_of(half * hidden, 128), hidden)
    given = pl.ds(pl.multiple_of((1 - half) * hidden, 128), hidden)

    loads = {}
    for n, (key, src, dst) in enumerate(
        (
            ("value", value_hbm, value_v),
            ("step", step_hbm, step_v),
            ("gate", gate_hbm, gate_v),
            ("outw", outw_hbm, outw_v),
            ("res", res_hbm.at[pl.ds(pl.multiple_of(tp * own, own), own), :], res_v),
            ("up", up_hbm.at[:, kept], up_all.at[pl.ds(pl.multiple_of(me * piece, piece), piece), :]),
            ("down", down_hbm.at[:, kept], down_all.at[pl.ds(pl.multiple_of(me * piece, piece), piece), :]),
        )
    ):
        loads[key] = pltpu.make_async_copy(src, dst, local_sem.at[n])
        loads[key].start()

    barrier = pltpu.get_barrier_semaphore()
    for d in range(1, n_sp):
        pl.semaphore_signal(
            barrier, inc=1, device_id=(lax.rem(me + d, n_sp), tp), device_id_type=MESH
        )
    for d in range(1, n_tp):
        pl.semaphore_signal(
            barrier, inc=1, device_id=(me, lax.rem(tp + d, n_tp)), device_id_type=MESH
        )
    pl.semaphore_wait(barrier, n_sp + n_tp - 2)

    started = {}

    def guarded(cond, act_on):
        if cond is None:
            act_on()
        else:
            pl.when(cond)(act_on)

    def launch(key, src, dst, target, send_if=None, recv_if=None):
        copy = pltpu.make_async_remote_copy(
            src_ref=src, dst_ref=dst, send_sem=send.at[ids[key]], recv_sem=recv.at[ids[key]],
            device_id=target, device_id_type=MESH,
        )
        guarded(send_if, copy.start)
        started[key] = (copy, send_if, recv_if)

    def take(key):
        copy, _, recv_if = started[key]
        guarded(recv_if, copy.wait_recv)

    streams = {
        "u": (up_hbm, False, up_all),
        "v": (up_hbm, True, up_all),
        "c": (down_hbm, False, down_all),
        "e": (down_hbm, True, down_all),
    }

    def landed(name, source):
        _, far, buf = streams[name]
        if far:
            source = lax.rem(source + half_size, n_sp)
        return buf.at[pl.ds(pl.multiple_of(source * piece, 16), piece), :]

    def origin(name):
        hbm, far, _ = streams[name]
        return landed(name, me) if far else hbm.at[:, kept]

    def has(k, sign):
        return hi >= k if sign > 0 else hi + k < high

    def line(name, k):
        for sign in (1, -1):
            dst = landed(name, at(-sign * (k - 1), "o"))
            src = origin(name) if k == 1 else dst
            onward = hi + 1 < high if sign > 0 else hi >= 1
            send_if = onward if k == 1 else jnp.logical_and(onward, has(k - 1, sign))
            launch((name, "o", k, sign), src, dst, (above if sign > 0 else below, tp),
                   send_if, has(k, sign))

    def across(name):
        launch((name, "x"), origin(name), landed(name, me), (beside, tp))

    def forward(name, k):
        for sign in (1, -1):
            take((name, "o", k, sign))
        if k < high - 1:
            line(name, k + 1)
        for sign in (1, -1):
            view = landed(name, at(-sign * k, "o"))
            launch((name, "f", k, sign), view, view, (beside, tp), has(k, sign), has(k, sign))

    halo_copy_key = ("halo",)
    launch(
        halo_copy_key, value_hbm.at[pl.ds(rows - 16, 16), :], halo,
        (lax.rem(me + 1, n_sp), tp),
    )
    mine_up = up_all.at[pl.ds(pl.multiple_of(me * piece, 16), piece), :]
    mine_down = down_all.at[pl.ds(pl.multiple_of(me * piece, 16), piece), :]
    launch(("pu",), up_hbm.at[:, given], mine_up, (partner, tp))
    line("u", 1)
    across("u")
    launch(("pd",), down_hbm.at[:, given], mine_down, (partner, tp))
    line("c", 1)
    across("c")

    bw = rate_ref.shape[1]
    per = 128 // bw
    groups = ch // 128
    r_i = lax.broadcasted_iota(jnp.int32, (bw, 128), 0)
    c_i = lax.broadcasted_iota(jnp.int32, (bw, 128), 1)
    for g in range(groups):
        for which, ref in ((0, rate_ref), (1, inp_ref)):
            for j in range(per):
                place = jnp.where(c_i == r_i + j * bw, 1.0, 0.0).astype(BF16)
                block = jnp.dot(ref[g * per + j], place, preferred_element_type=F32)
                wpair[which, g, j * bw : (j + 1) * bw, :] = block.astype(BF16)

    loads["value"].wait()
    loads["step"].wait()
    take(halo_copy_key)
    taps = conv_ref.shape[0]
    first = jnp.where(me == 0, 0.0, 1.0).astype(F32)
    pad[0:8, :] = halo[8:16, :].astype(F32) * first

    chunk = 64

    def widen(r, c):
        at_row = pl.multiple_of(r * chunk, chunk)
        pad[pl.ds(pl.multiple_of(at_row + 8, 8), chunk), :] = value_v[
            pl.ds(at_row, chunk), :
        ].astype(F32)
        return c

    lax.fori_loop(0, rows // chunk, widen, 0)

    def gates(r, c):
        at_row = pl.multiple_of(r * chunk, chunk)
        for g in range(groups):
            lanes = slice(g * 128, (g + 1) * 128)
            window = pad[pl.ds(at_row, chunk + 8), lanes]
            total = jnp.zeros((chunk, 128), F32)
            for k in range(taps):
                shift = 8 - taps + 1 + k
                moved = window if shift == 0 else pltpu.roll(window, chunk + 8 - shift, 0)
                total = total + moved[0:chunk, :] * conv_ref[k : k + 1, lanes]
            smooth = total.astype(BF16)
            rate = lax.logistic(jnp.dot(smooth, wpair[0, g], preferred_element_type=F32))
            gate = lax.logistic(jnp.dot(smooth, wpair[1, g], preferred_element_type=F32))
            log_keep = -8.0 * step_v[pl.ds(at_row, chunk), lanes] * rate * decay_ref[0:1, lanes]
            keep[g, pl.ds(at_row, chunk), :] = jnp.exp(log_keep)
            drive[g, pl.ds(at_row, chunk), :] = (
                jnp.sqrt(one_minus_exp(2.0 * log_keep)) * gate * smooth.astype(F32)
            )
        return c

    lax.fori_loop(0, rows // chunk, gates, 0)

    seg = rows // SCAN

    def scan(i, carry):
        p, h = carry
        idx = pl.ds(i, SCAN, stride=seg)
        new_p, new_h = [], []
        for g in range(groups):
            a, d = keep[g, idx, :], drive[g, idx, :]
            hg = a * h[g] + d
            pg = a * p[g]
            keep[g, idx, :] = pg
            drive[g, idx, :] = hg
            new_p.append(pg)
            new_h.append(hg)
        return tuple(new_p), tuple(new_h)

    ones = tuple(jnp.ones((SCAN, 128), F32) for _ in range(groups))
    zeros = tuple(jnp.zeros((SCAN, 128), F32) for _ in range(groups))
    lax.fori_loop(0, seg, scan, (ones, zeros))

    def pick(ref, row):
        return jnp.concatenate([ref[g, row : row + 1, :] for g in range(groups)], axis=1)

    ends = [(pick(keep, (b + 1) * seg - 1), pick(drive, (b + 1) * seg - 1)) for b in range(SCAN)]
    whole_p, whole_h = ends[0]
    for p_b, h_b in ends[1:]:
        whole_p, whole_h = whole_p * p_b, p_b * whole_h + h_b
    row_id = lax.broadcasted_iota(jnp.int32, (8, ch), 0)
    tot[me] = jnp.where(row_id == 0, whole_p, whole_h)
    carries = []
    for d in range(1, n_sp):
        copy = pltpu.make_async_remote_copy(
            src_ref=tot.at[me], dst_ref=tot.at[me], send_sem=csend.at[d], recv_sem=crecv.at[d],
            device_id=(lax.rem(me + d, n_sp), tp), device_id_type=MESH,
        )
        copy.start()
        carries.append(copy)
    loads["gate"].wait()
    loads["outw"].wait()
    for copy in carries:
        copy.wait_recv()

    def fold(d, s):
        joined = tot[d, 0:1, :] * s + tot[d, 1:2, :]
        return jnp.where(d < me, joined, s)

    state = lax.fori_loop(0, n_sp, fold, jnp.zeros((1, ch), F32))
    for b in range(SCAN):
        ent[b, 0:1, :] = state
        state = ends[b][0] * state + ends[b][1]

    def gating(b, c):
        at_row = pl.ds(pl.multiple_of(b * seg, seg), seg)
        for g in range(groups):
            lanes = slice(g * 128, (g + 1) * 128)
            full = drive[g, at_row, :] + keep[g, at_row, :] * ent[b, 0:1, lanes]
            branch = jax.nn.gelu(gate_v[at_row, lanes].astype(F32), approximate=True)
            gated[at_row, lanes] = (branch * full).astype(BF16)
        return c

    lax.fori_loop(0, SCAN, gating, 0)

    sums = []
    for d in list(range(1, n_tp)) + [0]:
        peer = lax.rem(tp + d, n_tp)
        span = pl.ds(pl.multiple_of(peer * own, own), own)
        part[span, :] = jnp.dot(gated[span, :], outw_v[...], preferred_element_type=F32).astype(BF16)
        if d:
            copy = pltpu.make_async_remote_copy(
                src_ref=part.at[span, :], dst_ref=part_in.at[tp],
                send_sem=tsend.at[0, d], recv_sem=trecv.at[0, d],
                device_id=(me, peer), device_id_type=MESH,
            )
            copy.start()
            sums.append(copy)

    take(("pu",))
    line("v", 1)
    across("v")
    forward("u", 1)

    mine = pl.ds(pl.multiple_of(tp * own, own), own)
    loads["res"].wait()
    for copy in sums:
        copy.wait_recv()
    slab = 32

    def settle(r, c):
        here = pl.ds(pl.multiple_of(r * slab, slab), slab)
        there = pl.ds(pl.multiple_of(tp * own + r * slab, slab), slab)
        mixed = part[there, :].astype(F32)
        for d in range(1, n_tp):
            mixed = mixed + part_in[lax.rem(tp + d, n_tp), here, :].astype(F32)
        new = (res_v[here, :].astype(F32) + mixed).astype(BF16)
        upd[here, :] = new
        wide = new.astype(F32)
        factor = lax.rsqrt(jnp.mean(wide * wide, axis=-1, keepdims=True) + 1e-06)
        normed[there, :] = (wide * factor * gain_ref[0:1, :]).astype(BF16)
        return c

    lax.fori_loop(0, own // slab, settle, 0)
    shares = []
    far_mine = pl.ds(pl.multiple_of(rows + tp * own, own), own)
    launch(("n",), normed.at[mine, :], normed.at[far_mine, :], (partner, tp))

    pairs = n_tp // 2
    pair, side_of = tp // 2, lax.rem(tp, 2)
    mate = pair * 2 + 1 - side_of

    def share_to(owner, base, turn, n, target):
        span = pl.ds(pl.multiple_of(base + owner * own, own), own)
        copy = pltpu.make_async_remote_copy(
            src_ref=normed.at[span, :], dst_ref=normed.at[span, :],
            send_sem=tsend.at[turn, n], recv_sem=trecv.at[turn, n],
            device_id=(me, target), device_id_type=MESH,
        )
        copy.start()
        return copy

    def share(base, turn):
        copies = [
            share_to(tp, base, turn, j, lax.rem(tp + 2 * j, n_tp)) for j in range(1, pairs)
        ]
        return [share_to(tp, base, turn, 0, mate)] + copies

    def pass_on(copies, base, turn):
        more = []
        for j in range(1, pairs):
            copies[j].wait_recv()
            owner = lax.rem(tp - 2 * j + n_tp, n_tp)
            more.append(share_to(owner, base, turn, pairs - 1 + j, mate))
        return more

    shares = share(0, 1)
    take(("pd",))
    line("e", 1)
    across("e")
    forward("c", 1)
    forward("v", 1)
    passed = pass_on(shares, 0, 1)
    take(("n",))
    shares_far = share(rows, 2)
    forward("e", 1)
    for k in range(2, high):
        for name in ("u", "v", "c", "e"):
            forward(name, k)
    loads["up"].wait()
    loads["down"].wait()

    def settle_stream(name):
        take((name, "x"))
        for k in range(1, high):
            for sign in (1, -1):
                take((name, "f", k, sign))

    passed_far = pass_on(shares_far, rows, 2)
    settle_stream("u")
    settle_stream("v")
    tile = 512

    for copy in shares[:1] + passed:
        copy.wait_recv()
    def raise_rows(start):
        def one(n, c):
            cols = pl.ds(pl.multiple_of(n * tile, tile), tile)
            lifted = jnp.dot(
                normed[start : start + rows, :], up_all[:, cols], preferred_element_type=F32
            )
            lifted = jnp.maximum(lifted, 0.0)
            act[start : start + rows, cols] = (lifted * lifted).astype(BF16)
            return c

        lax.fori_loop(0, hidden // tile, one, 0)

    raise_rows(0)
    for copy in shares_far[:1] + passed_far:
        copy.wait_recv()
    raise_rows(rows)
    settle_stream("c")
    settle_stream("e")
    blocks = width // tile
    lowered = {}

    def lower(side, q):
        cols = slice(q * tile, (q + 1) * tile)
        base = side * rows
        fin[base : base + rows, cols] = lax.dot_general(
            act[base : base + rows, :], down_all[cols, :], (((1,), (1,)), ((), ())),
            preferred_element_type=F32,
        ).astype(BF16)
        for i in range(pairs):
            there = pl.ds(pl.multiple_of(base + (2 * i + 1 - side_of) * own, own), own)
            copy = pltpu.make_async_remote_copy(
                src_ref=fin.at[there, cols], dst_ref=pair_in.at[side, i, :, cols],
                send_sem=fsend.at[side * blocks + q, i], recv_sem=frecv.at[side * blocks + q, i],
                device_id=(me, mate), device_id_type=MESH,
            )
            copy.start()
            lowered[side, q, i] = copy

    def combine(side, q):
        cols = slice(q * tile, (q + 1) * tile)
        for i in range(pairs):
            lowered[side, q, i].wait_recv()
        for j in range(1, pairs):
            peer = lax.rem(tp + 2 * j, n_tp)
            start = pl.multiple_of(side * rows + peer * own, own)

            def add(r, c, start=start, peer=peer):
                here = pl.ds(pl.multiple_of(r * slab, slab), slab)
                there = pl.ds(pl.multiple_of(start + r * slab, slab), slab)
                fin[there, cols] = (
                    fin[there, cols].astype(F32)
                    + pair_in[side, peer // 2, here, cols].astype(F32)
                ).astype(BF16)
                return c

            lax.fori_loop(0, own // slab, add, 0)
            n = pairs - 1 + j
            copy = pltpu.make_async_remote_copy(
                src_ref=fin.at[pl.ds(start, own), cols],
                dst_ref=fin_in.at[pair, side * own : (side + 1) * own, cols],
                send_sem=fsend.at[side * blocks + q, n], recv_sem=frecv.at[side * blocks + q, n],
                device_id=(me, peer), device_id_type=MESH,
            )
            copy.start()
            lowered[side, q, n] = copy

    def gathered(side, r, cols):
        here = pl.ds(pl.multiple_of(side * own + r * slab, slab), slab)
        near = pl.ds(pl.multiple_of(r * slab, slab), slab)
        there = pl.ds(pl.multiple_of(side * rows + tp * own + r * slab, slab), slab)
        total = fin[there, cols].astype(F32) + pair_in[side, pair, near, cols].astype(F32)
        for j in range(1, pairs):
            total = total + fin_in[lax.rem(pair + j, pairs), here, cols].astype(F32)
        return total

    for side in (1, 0):
        for q in range(blocks):
            lower(side, q)
        for q in range(blocks):
            combine(side, q)
    for q in range(blocks):
        cols = slice(q * tile, (q + 1) * tile)
        for j in range(1, pairs):
            lowered[1, q, pairs - 1 + j].wait_recv()

        def far_sum(r, c, cols=cols):
            here = pl.ds(pl.multiple_of(r * slab, slab), slab)
            far_out[here, cols] = gathered(1, r, cols).astype(BF16)
            return c

        lax.fori_loop(0, own // slab, far_sum, 0)
        launch(("r", q), far_out.at[:, cols], far_in.at[:, cols], (partner, tp))
    for q in range(blocks):
        cols = slice(q * tile, (q + 1) * tile)
        for j in range(1, pairs):
            lowered[0, q, pairs - 1 + j].wait_recv()
        take(("r", q))

        def finish(r, c, cols=cols):
            here = pl.ds(pl.multiple_of(r * slab, slab), slab)
            total = gathered(0, r, cols) + far_in[here, cols].astype(F32)
            out_ref[here, cols] = (upd[here, cols].astype(F32) + total).astype(BF16)
            return c

        lax.fori_loop(0, own // slab, finish, 0)
    for copy, send_if, _ in started.values():
        guarded(send_if, copy.wait_send)
    for copy in carries + sums + shares + shares_far + passed + passed_far + list(lowered.values()):
        copy.wait_send()


def copy_ids(n_sp, blocks):
    keys = [("pu",), ("pd",), ("halo",), ("n",)] + [("r", q) for q in range(blocks)]
    for name in ("u", "v", "c", "e"):
        keys.append((name, "x"))
        for k in range(1, n_sp // 4):
            for sign in (1, -1):
                keys += [(name, "o", k, sign), (name, "f", k, sign)]
    return {key: n for n, key in enumerate(keys)}


def solution(mesh):
    n_sp, n_tp = mesh.shape["sp"], mesh.shape["tp"]

    def local(res, gate, value, conv, rate, inp, decay, step, outw, gain, up, down):
        rows, ch = value.shape
        width, hidden = outw.shape[1], up.shape[1]
        own = rows // n_tp
        hidden = hidden // 2
        ids = copy_ids(n_sp, width // 512)
        V = pltpu.VMEM
        any_spec = pl.BlockSpec(memory_space=pl.ANY)
        vm = pl.BlockSpec(memory_space=pltpu.VMEM)
        dma = pltpu.SemaphoreType.DMA
        return pl.pallas_call(
            functools.partial(kernel, (n_sp, n_tp, ids)),
            out_shape=jax.ShapeDtypeStruct((own, width), BF16),
            in_specs=[any_spec, any_spec, any_spec, vm, vm, vm, vm, any_spec, any_spec, vm,
                      any_spec, any_spec],
            out_specs=vm,
            scratch_shapes=[
                V((width, hidden), BF16), V((width, hidden), BF16),
                V((2 * rows, hidden), BF16), V((2 * rows, width), BF16),
                V((rows, width), BF16), V((n_tp, own, width), BF16),
                V((2 * rows, width), BF16), V((n_tp // 2, 2 * own, width), BF16),
                V((2, n_tp // 2, own, width), BF16),
                V((own, width), BF16), V((own, width), BF16),
                V((ch // 128, rows, 128), F32), V((ch // 128, rows, 128), F32), V((rows + 8, ch), F32),
                V((rows, ch), BF16), V((rows, ch), BF16), V((rows, ch), BF16),
                V((rows, ch), F32), V((ch, width), BF16), V((own, width), BF16),
                V((16, ch), BF16), V((n_sp, 8, ch), F32), V((SCAN, 8, ch), F32),
                V((own, width), BF16), V((2, ch // 128, 128, 128), BF16),
                dma((len(ids),)), dma((len(ids),)), dma((3, n_tp)), dma((3, n_tp)),
                dma((2 * width // 512, n_tp)), dma((2 * width // 512, n_tp)),
                dma((n_sp,)), dma((n_sp,)), dma((7,)),
            ],
            compiler_params=pltpu.CompilerParams(
                collective_id=0, has_side_effects=True, vmem_limit_bytes=62 * 1024 * 1024
            ),
        )(res, gate, value, conv, rate, inp, decay.reshape(1, -1), step, outw,
          gain.reshape(1, -1), up, down)

    in_specs = (
        P("sp", None), P("sp", "tp"), P("sp", "tp"), P(None, "tp"),
        P("tp", None, None), P("tp", None, None), P("tp"), P("sp", "tp"),
        P("tp", None), P(), P("sp", "tp"), P("sp", "tp"),
    )
    return jax.shard_map(
        local, mesh=mesh, in_specs=in_specs, out_specs=P(("sp", "tp"), None), check_vma=False
    )
```
